32 devices in a mesh: sp: 8 (over z, y), tp: 4 (over x, core).
Axes of the slice: x: 2, y: 2, z: 4, core: 2. Of those that a mesh axis runs over, the one named last changes fastest.
Arguments:
- resid_in: bfloat16 [1024, 2048], P('sp'), may hold values from -6 to 6
- query_plain: bfloat16 [1024, 2048], P('sp', 'tp'), may hold values from -480 to 480, as said below
- query_turn: bfloat16 [1024, 1024], P('sp', 'tp'), may hold values from -16 to 16
- latent_raw: bfloat16 [1024, 256], P('sp'), may hold values from -6 to 6
- shared_key: bfloat16 [1024, 32], P('sp'), may hold values from -6 to 6
- latent_gain: float32 [256], replicated, may hold values from 0.1 to 1.9
- key_up: bfloat16 [256, 2048], P(None, 'tp'), may hold values from -0.375 to 0.375
- value_up: bfloat16 [256, 2048], P(None, 'tp'), may hold values from -0.375 to 0.375
- out_weight: bfloat16 [2048, 2048], P('tp'), may hold values from -0.5 to 0.5
- mixer_gain: float32 [2048], replicated, may hold values from 0.1 to 1.9
- gate_weight: bfloat16 [2048, 5632], P('sp', 'tp'), may hold values from -0.125 to 0.125
- up_weight: bfloat16 [2048, 5632], P('sp', 'tp'), may hold values from -0.125 to 0.125
- down_weight: bfloat16 [5632, 2048], P('tp', 'sp'), may hold values from -0.15625 to 0.15625
Outputs:
- layer_out: bfloat16 [1024, 2048], P(('sp', 'tp'))
The draws below stay inside these ranges and needn't reach their ends.
Inputs may be any that keep to these rules, and one draw needn't show every extreme that they name: Entries of query_plain lie in this range.
All inputs are finite; a program needn't handle non-finite values.
Results may differ from the reference program's by a relative error of at most 0.014.
The reference program's roundings to bfloat16 on the way (of `query_rot`, `key_rot`, `latent`, `weight`, `attended`, `normed` and `hidden`) count: a program that leaves them out, or rounds other values in their place, can miss the bound.
Values may be sent and summed in bfloat16 or wider, within the bound.
A program may use at most 128 MiB of HBM per device.

```python
import math
import jax
import jax.numpy as jnp
from jax import lax

D = 2048
H = 32
NOPE = 64
ROPE = 32
V = 64
KV = 256
FF = 5632
HV = 2048
TOKENS = 1024


def draw_query_plain(key, part):
    first = jax.random.fold_in(jax.random.fold_in(key, 11), 0)
    base = jnp.clip(jax.random.normal(first, (TOKENS, H * NOPE), jnp.float32), -6.0, 6.0) * 2.5
    return base.astype(jnp.bfloat16)


def level_of(key, shape, cuts, least, top_value):
    def one(dim, parts):
        heights = jax.random.uniform(jax.random.fold_in(jax.random.fold_in(key, 6), dim), (parts,), jnp.float32, least / len(cuts), top_value / len(cuts))
        return jnp.repeat(jnp.exp(heights), shape[dim] // parts).reshape((-1,) + (1,) * (len(shape) - dim - 1))

    factor_of = one(*cuts[0])
    for cut in cuts[1:]:
        factor_of = factor_of * one(*cut)
    return factor_of


def scatter_about(key, dims, spread, limit, cuts=(), held_as=jnp.bfloat16):
    result = spread * jax.random.normal(key, dims, jnp.float32)
    if cuts:
        result = result * level_of(key, dims, cuts, -0.22, 0.18)
    return jnp.clip(result, -limit, limit).astype(held_as)


def setup_inputs(seed: int = 0) -> dict:
    keys = jax.random.split(jax.random.key(seed), 14)
    resid_in = scatter_about(keys[0], (TOKENS, D), 1.0, 6.0, ((0, 8),))
    query_plain = draw_query_plain(jax.random.fold_in(keys[13], 71), 0)
    query_turn = scatter_about(keys[2], (TOKENS, H * ROPE), 2.5, 16.0, ((0, 8), (1, 4)))
    latent_raw = scatter_about(keys[3], (TOKENS, KV), 1.0, 6.0, ((0, 8),))
    shared_key = scatter_about(keys[4], (TOKENS, ROPE), 1.0, 6.0, ((0, 8),))
    latent_gain = jnp.clip(1.0 + 0.18 * jax.random.normal(keys[5], (KV,), jnp.float32), 0.1, 1.9)
    key_up = scatter_about(keys[6], (KV, H * NOPE), KV ** -0.5, 0.375, ((1, 4),))
    value_up = scatter_about(keys[7], (KV, HV), KV ** -0.5, 0.375, ((1, 4),))
    out_weight = scatter_about(keys[8], (HV, D), (HV // 16) ** -0.5, 0.5, ((0, 4),))
    mixer_gain = jnp.clip(1.0 + 0.18 * jax.random.normal(keys[9], (D,), jnp.float32), 0.1, 1.9)
    gate_weight = scatter_about(keys[10], (D, FF), D ** -0.5, 0.125, ((0, 8), (1, 4)))
    up_weight = scatter_about(keys[11], (D, FF), D ** -0.5, 0.125, ((0, 8), (1, 4)))
    down_weight = scatter_about(keys[12], (FF, D), (FF // 4) ** -0.5, 0.15625, ((0, 4), (1, 8)))
    return dict(resid_in=resid_in, query_plain=query_plain, query_turn=query_turn, latent_raw=latent_raw, shared_key=shared_key, latent_gain=latent_gain, key_up=key_up, value_up=value_up, out_weight=out_weight, mixer_gain=mixer_gain, gate_weight=gate_weight, up_weight=up_weight, down_weight=down_weight)


def rotate(values, cosine, sine):
    half_width = values.shape[-1] // 2
    first = values[..., :half_width]
    second = values[..., half_width:]
    return jnp.concatenate([first * cosine - second * sine, first * sine + second * cosine], axis=-1)

def rms_scale(values, gain):
    return values * lax.rsqrt(lax.optimization_barrier(jnp.mean(values * values, axis=-1, keepdims=True)) + 1e-06) * gain.astype(jnp.float32)

def reference(resid_in, query_plain, query_turn, latent_raw, shared_key, latent_gain, key_up, value_up, out_weight, mixer_gain, gate_weight, up_weight, down_weight):
    position = jnp.arange(TOKENS, dtype=jnp.int32).astype(jnp.float32)
    inverse = 10000.0 ** (-jnp.arange(0, ROPE, 2, dtype=jnp.float32) / ROPE)
    angles = position[:, None] * inverse[None, :]
    cosine = jnp.cos(angles)
    sine = jnp.sin(angles)
    query_rot = rotate(query_turn.astype(jnp.float32).reshape(TOKENS, H, ROPE), cosine[:, None, :], sine[:, None, :]).astype(jnp.bfloat16)
    key_rot = rotate(shared_key.astype(jnp.float32), cosine, sine).astype(jnp.bfloat16)
    latent = rms_scale(latent_raw.astype(jnp.float32), latent_gain).astype(jnp.bfloat16)
    key_plain = jnp.dot(latent, key_up, preferred_element_type=jnp.float32).astype(jnp.bfloat16).reshape(TOKENS, H, NOPE)
    values = jnp.dot(latent, value_up, preferred_element_type=jnp.float32).astype(jnp.bfloat16).reshape(TOKENS, H, V)
    query_heads = query_plain.reshape(TOKENS, H, NOPE)
    block_len = math.gcd(TOKENS, 128)
    block_count = TOKENS // block_len
    scale = (NOPE + ROPE) ** (-0.5)
    key_plain32 = key_plain.astype(jnp.float32)
    key_rot32 = key_rot.astype(jnp.float32)
    values32 = values.astype(jnp.float32)

    def attend(blocks):
        query_block, rot_block = blocks
        score = jnp.einsum('qhd,khd->hqk', query_block.astype(jnp.float32), key_plain32)
        score = score + jnp.einsum('qhr,kr->hqk', rot_block.astype(jnp.float32), key_rot32)
        score = score * scale
        top = lax.optimization_barrier(jnp.max(score, axis=-1, keepdims=True))
        expo = jnp.exp(score - top)
        total = lax.optimization_barrier(jnp.sum(expo, axis=-1))
        weight = expo.astype(jnp.bfloat16).astype(jnp.float32)
        summed = jnp.einsum('hqk,khd->qhd', weight, values32)
        return (summed / total.T[:, :, None]).astype(jnp.bfloat16)
    attended = lax.map(attend, (query_heads.reshape(block_count, block_len, H, NOPE), query_rot.reshape(block_count, block_len, H, ROPE)))
    attended = attended.reshape(TOKENS, H * V)
    mid = resid_in.astype(jnp.float32) + jnp.dot(attended, out_weight, preferred_element_type=jnp.float32)
    normed = rms_scale(mid, mixer_gain).astype(jnp.bfloat16)
    gate_sum = jnp.dot(normed, gate_weight, preferred_element_type=jnp.float32)
    up_sum = jnp.dot(normed, up_weight, preferred_element_type=jnp.float32)
    hidden = (jax.nn.silu(gate_sum) * up_sum).astype(jnp.bfloat16)
    down_sum = jnp.dot(hidden, down_weight, preferred_element_type=jnp.float32)
    return (mid + 0.5 * down_sum).astype(jnp.bfloat16)
```

```python
import functools
import math

import jax
import jax.numpy as jnp
from jax import lax
from jax.experimental import pallas as pl
from jax.experimental.pallas import tpu as pltpu
from jax.sharding import PartitionSpec as P

NOPE = 64
ROPE = 32
V = 64


def rotate(values, cosine, sine):
    half_width = values.shape[-1] // 2
    first = values[..., :half_width]
    second = values[..., half_width:]
    return jnp.concatenate(
        [first * cosine - second * sine, first * sine + second * cosine], axis=-1
    )


def rms_scale(values, gain):
    return values * lax.rsqrt(jnp.mean(values * values, axis=-1, keepdims=True) + 1e-06) * gain


def plain_layer(
    resid_in,
    query_plain,
    query_turn,
    latent_raw,
    shared_key,
    latent_gain,
    key_up,
    value_up,
    out_weight,
    mixer_gain,
    gate_weight,
    up_weight,
    down_weight,
):
    tok_rows = resid_in.shape[0]
    head_count = query_plain.shape[1] // NOPE
    part_rows = tok_rows // lax.axis_size("tp")
    offset = lax.axis_index("sp") * tok_rows
    position = (offset + jnp.arange(tok_rows, dtype=jnp.int32)).astype(jnp.float32)
    inverse = 10000.0 ** (-jnp.arange(0, ROPE, 2, dtype=jnp.float32) / ROPE)
    angles = position[:, None] * inverse[None, :]
    cosine = jnp.cos(angles)
    sine = jnp.sin(angles)
    query_heads = query_plain.reshape(tok_rows, head_count, NOPE)
    query_rot = rotate(
        query_turn.reshape(tok_rows, head_count, ROPE).astype(jnp.float32),
        cosine[:, None, :],
        sine[:, None, :],
    ).astype(jnp.bfloat16)
    latent = rms_scale(latent_raw.astype(jnp.float32), latent_gain).astype(jnp.bfloat16)
    key_rot = rotate(shared_key.astype(jnp.float32), cosine, sine).astype(jnp.bfloat16)
    softmax_scale = (NOPE + ROPE) ** (-0.5)

    def attend_block(state, key_plain, values, key_pos):
        run_max, run_total, run_acc = state
        score = jnp.einsum(
            "qhd,khd->hqk", query_heads, key_plain, preferred_element_type=jnp.float32
        )
        score = score + jnp.einsum(
            "qhr,kr->hqk", query_rot, key_pos, preferred_element_type=jnp.float32
        )
        score = score * softmax_scale
        new_max = jnp.maximum(run_max, jnp.max(score, axis=-1))
        shrink = jnp.exp(run_max - new_max)
        expo = jnp.exp(score - new_max[:, :, None])
        run_total = run_total * shrink + jnp.sum(expo, axis=-1)
        run_acc = run_acc * shrink.T[:, :, None] + jnp.einsum(
            "hqk,khd->qhd", expo.astype(jnp.bfloat16), values, preferred_element_type=jnp.float32
        )
        return (new_max, run_total, run_acc)

    start_state = (
        jnp.full((head_count, tok_rows), -jnp.inf, jnp.float32),
        jnp.zeros((head_count, tok_rows), jnp.float32),
        jnp.zeros((tok_rows, head_count, V), jnp.float32),
    )
    state = start_state
    latent_piece = lax.all_gather(latent, "sp", axis=0, tiled=True)
    pos_piece = lax.all_gather(key_rot, "sp", axis=0, tiled=True)
    piece_len = latent_piece.shape[0]
    block_len = math.gcd(piece_len, 512)
    block_count = piece_len // block_len

    def one_block(inner, items):
        latent_rows, pos_rows = items
        key_plain = (
            jnp.dot(latent_rows, key_up, preferred_element_type=jnp.float32)
            .astype(jnp.bfloat16)
            .reshape(block_len, head_count, NOPE)
        )
        values = (
            jnp.dot(latent_rows, value_up, preferred_element_type=jnp.float32)
            .astype(jnp.bfloat16)
            .reshape(block_len, head_count, V)
        )
        return (attend_block(inner, key_plain, values, pos_rows), None)

    state, unused = lax.scan(
        one_block,
        state,
        (
            latent_piece.reshape(block_count, block_len, latent_piece.shape[1]),
            pos_piece.reshape(block_count, block_len, ROPE),
        ),
    )
    attended = (
        (state[2] / state[1].T[:, :, None]).astype(jnp.bfloat16).reshape(tok_rows, head_count * V)
    )
    own_start = lax.axis_index("tp") * part_rows
    mixed = lax.psum_scatter(
        jnp.dot(attended, out_weight, preferred_element_type=jnp.float32).astype(jnp.bfloat16),
        "tp",
        scatter_dimension=0,
        tiled=True,
    ).astype(jnp.float32)
    middle = lax.dynamic_slice_in_dim(resid_in, own_start, part_rows, 0).astype(jnp.float32) + mixed
    normed = rms_scale(middle, mixer_gain).astype(jnp.bfloat16)
    all_rows = lax.all_gather(normed, "tp", axis=0, tiled=True)
    gate_sum = jnp.dot(
        all_rows,
        lax.all_gather(gate_weight, "sp", axis=0, tiled=True),
        preferred_element_type=jnp.float32,
    )
    up_sum = jnp.dot(
        all_rows,
        lax.all_gather(up_weight, "sp", axis=0, tiled=True),
        preferred_element_type=jnp.float32,
    )
    hidden = (jax.nn.silu(gate_sum) * up_sum).astype(jnp.bfloat16)
    terms = jnp.dot(
        hidden,
        lax.all_gather(down_weight, "sp", axis=1, tiled=True),
        preferred_element_type=jnp.float32,
    )
    down_sum = lax.psum_scatter(
        terms.astype(jnp.bfloat16), "tp", scatter_dimension=0, tiled=True
    ).astype(jnp.float32)
    return (middle + 0.5 * down_sum).astype(jnp.bfloat16)

MESH = pl.DeviceIdType.MESH
BF = jnp.bfloat16
F32 = jnp.float32
BY_LAST = (((1,), (1,)), ((), ()))


def turn(values, cosine, sine):
    width = values.shape[-1]
    half = ROPE // 2
    lane = lax.broadcasted_iota(jnp.int32, values.shape, 1) % ROPE
    swapped = jnp.where(lane < half, pltpu.roll(values, width - half, 1), pltpu.roll(values, half, 1))
    return values * cosine + swapped * sine


def layer_kernel(
    sizes,
    resid_ref,
    query_ref,
    turn_ref,
    latent_ref,
    shared_ref,
    cos_ref,
    sin_ref,
    lgain_ref,
    kup_ref,
    vup_ref,
    ow_ref,
    mgain_ref,
    send_ref,
    out_ref,
    kv_buf,
    key_buf,
    val_buf,
    att_buf,
    mix_buf,
    mixb_buf,
    mixr_buf,
    mid_buf,
    w_buf,
    n_buf,
    p_buf,
    r1_buf,
    acc_buf,
    r_buf,
    w_ssem,
    w_rsem,
    w_lsem,
    l_ssem,
    l_rsem,
    f_ssem,
    f_rsem,
    m_ssem,
    m_rsem,
    a_ssem,
    a_rsem,
    d_ssem,
    d_rsem,
    c_ssem,
    c_rsem,
    s_ssem,
    s_rsem,
):
    sp, tp, zs, ys, xs = sizes
    s = lax.axis_index("sp")
    t = lax.axis_index("tp")
    core = t % 2
    other = t + 1 - 2 * core
    me = (s // ys, s % ys, t // 2)
    dims = (zs, ys, xs)
    rows = latent_ref.shape[0]
    part = rows // tp
    hid = send_ref.shape[1] // 3
    cols = send_ref.shape[2]
    kv_width = latent_ref.shape[1]

    def remote(src, dst, ssem, rsem, dev):
        return pltpu.make_async_remote_copy(
            src_ref=src, dst_ref=dst, send_sem=ssem, recv_sem=rsem, device_id=dev, device_id_type=MESH
        )

    sends = []

    lat = latent_ref[...].astype(F32)
    lat = lat * lax.rsqrt(jnp.mean(lat * lat, axis=-1, keepdims=True) + 1e-06) * lgain_ref[...]
    cosine = cos_ref[...]
    sine = sin_ref[...]
    half_rows = rows // 2
    own_lat = lat.astype(BF)
    own_key = turn(shared_ref[...].astype(F32), cosine, sine).astype(BF)
    for half in range(2):
        part_of = slice(half * half_rows, (half + 1) * half_rows)
        kv_buf[0, half, :, :kv_width] = own_lat[part_of]
        kv_buf[0, half, :, kv_width:] = own_key[part_of]
    for k in range(1, sp):
        cp = remote(kv_buf.at[0, core], kv_buf.at[k, core], l_ssem.at[k], l_rsem.at[k], ((s + k) % sp, t))
        cp.start()
        sends.append(cp)
    w_slot = w_buf.at[:, pl.ds(pl.multiple_of(s * cols, cols), cols)]
    keep = pltpu.make_async_copy(send_ref.at[s], w_slot, w_lsem)
    keep.start()
    for k in range(1, sp):
        dest = (s + k) % sp
        cp = remote(send_ref.at[dest], w_slot, w_ssem.at[k], w_rsem.at[k], (dest, t))
        cp.start()
        sends.append(cp)

    def make_kv(k):
        piece = kv_buf[k].reshape(rows, kv_buf.shape[3])
        piece_lat = piece[:, :kv_width]
        key_buf[k * rows:(k + 1) * rows, :] = jnp.dot(
            piece_lat, kup_ref[...], preferred_element_type=F32
        ).astype(BF)
        val_buf[k * rows:(k + 1) * rows, :] = jnp.dot(
            piece_lat, vup_ref[...], preferred_element_type=F32
        ).astype(BF)

    make_kv(0)
    query_rot = turn(
        turn_ref[...].astype(F32),
        jnp.concatenate([cosine] * (turn_ref.shape[1] // cosine.shape[1]), axis=1),
        jnp.concatenate([sine] * (turn_ref.shape[1] // cosine.shape[1]), axis=1),
    ).astype(BF)
    for k in range(1, sp):
        remote(kv_buf.at[k, core], kv_buf.at[k, core], l_ssem.at[k], l_rsem.at[k], (s, other)).wait_recv()
        cp = remote(kv_buf.at[k, core], kv_buf.at[k, core], f_ssem.at[k], f_rsem.at[k], (s, other))
        cp.start()
        sends.append(cp)
    for k in range(1, sp):
        remote(
            kv_buf.at[k, 1 - core], kv_buf.at[k, 1 - core], f_ssem.at[k], f_rsem.at[k], (s, other)
        ).wait_recv()
        make_kv(k)

    scale = (NOPE + ROPE) ** (-0.5)
    all_rot = kv_buf[...].reshape(sp * rows, kv_buf.shape[3])[:, kv_width:]
    lane = lax.broadcasted_iota(jnp.int32, (rows, 128), 1)
    for pair in range(query_ref.shape[1] // 128):
        span = slice(pair * 128, (pair + 1) * 128)
        keys = jnp.concatenate([key_buf[:, span], all_rot], axis=1)
        vals = val_buf[:, span]
        results = []
        for inner in range(2):
            head = pair * 2 + inner
            tile = head * ROPE // 128
            group = head % (128 // ROPE)
            q_plain = jnp.where(lane // NOPE == inner, query_ref[:, span], jnp.zeros((), BF))
            q_turn = jnp.where(
                lane // ROPE == group, query_rot[:, tile * 128:(tile + 1) * 128], jnp.zeros((), BF)
            )
            score = lax.dot_general(
                jnp.concatenate([q_plain, q_turn], axis=1), keys, BY_LAST, preferred_element_type=F32
            ) * scale
            top = jnp.max(score, axis=-1, keepdims=True)
            expo = jnp.exp(score - top)
            total = jnp.sum(expo, axis=-1, keepdims=True)
            results.append(jnp.dot(expo.astype(BF), vals, preferred_element_type=F32) / total)
        att_buf[:, span] = jnp.where(lane < V, results[0], results[1]).astype(BF)

    mix_buf[...] = jnp.dot(att_buf[...], ow_ref[...], preferred_element_type=F32)
    mixb_buf[...] = mix_buf[...].astype(BF).reshape(mixb_buf.shape)
    for j in range(1, tp):
        dest = (t + j) % tp
        cp = remote(mixb_buf.at[dest], mixr_buf.at[j], m_ssem.at[j], m_rsem.at[j], (s, dest))
        cp.start()
        sends.append(cp)
    own_rows = pl.ds(pl.multiple_of(t * part, part), part)
    mid = resid_ref[own_rows, :].astype(F32) + mix_buf[own_rows, :]
    for j in range(1, tp):
        remote(mixb_buf.at[0], mixr_buf.at[j], m_ssem.at[j], m_rsem.at[j], (s, other)).wait_recv()
        mid = mid + mixr_buf[j].astype(F32)
    mid_buf[...] = mid
    normed = mid * lax.rsqrt(jnp.mean(mid * mid, axis=-1, keepdims=True) + 1e-06) * mgain_ref[...]
    index_of = lambda place: (place[0] * ys + place[1]) * xs + place[2]
    mine = index_of(me)
    n_buf[mine, core] = normed.astype(BF)

    def shifted(offset):
        return tuple((m + o) % n for m, o, n in zip(me, offset, dims))

    def device(offset):
        z, y, x = shifted(offset)
        return (z * ys + y, x * 2 + core)

    def along(d, k):
        return tuple(k if i == d else 0 for i in range(3))

    def plus(offset, d, k):
        return tuple((o + k) % dims[d] if i == d else o for i, o in enumerate(offset))

    def gather(order):
        held = [((0, 0, 0), -1)]
        out = []
        for stage, d in enumerate(order):
            for offset, _ in list(held):
                for k in range(1, dims[d]):
                    held.append((plus(offset, d, k), stage))
        for offset, stage in held:
            block = n_buf.at[index_of(shifted(offset)), core]
            if stage >= 0:
                i = index_of(offset)
                remote(block, block, a_ssem.at[i], a_rsem.at[i], (s, other)).wait_recv()
            for d in order[stage + 1:]:
                for k in range(1, dims[d]):
                    i = index_of(plus(offset, d, -k))
                    cp = remote(block, block, a_ssem.at[i], a_rsem.at[i], device(along(d, k)))
                    cp.start()
                    out.append(cp)
            i = index_of(offset)
            cp = remote(block, block, d_ssem.at[i], d_rsem.at[i], (s, other))
            cp.start()
            out.append(cp)
        for offset, _ in held:
            i = index_of(offset)
            block = n_buf.at[index_of(shifted(offset)), 1 - core]
            remote(block, block, d_ssem.at[i], d_rsem.at[i], (s, other)).wait_recv()
        for cp in out:
            cp.wait_send()

    @pl.when(core == 0)
    def _():
        gather((0, 1, 2))

    @pl.when(core == 1)
    def _():
        gather((2, 0, 1))

    keep.wait()
    for k in range(1, sp):
        remote(w_buf.at[:, :cols], w_buf.at[:, :cols], w_ssem.at[k], w_rsem.at[k], (s, other)).wait_recv()

    groups = n_buf.shape[0]
    step = groups // c_ssem.shape[0]

    def chunk(g, carry):
        some = pl.ds(g * step, step)
        block = n_buf[some].reshape(step * 2 * part, n_buf.shape[3])
        gate = lax.dot_general(block, w_buf[:hid], BY_LAST, preferred_element_type=F32)
        up = lax.dot_general(block, w_buf[hid:2 * hid], BY_LAST, preferred_element_type=F32)
        hidden = (gate / (1.0 + jnp.exp(-gate)) * up).astype(BF)
        down = jnp.dot(hidden, w_buf[2 * hid:], preferred_element_type=F32)
        p_buf[some] = down.astype(BF).reshape(step, 2, part, n_buf.shape[3])
        remote(p_buf.at[some, 1 - core], r1_buf.at[some], c_ssem.at[g], c_rsem.at[g], (s, other)).start()
        return carry

    lax.fori_loop(0, c_ssem.shape[0], chunk, 0)

    def join(g, carry):
        some = pl.ds(g * step, step)
        remote(p_buf.at[some, 1 - core], r1_buf.at[some], c_ssem.at[g], c_rsem.at[g], (s, other)).wait()
        acc_buf[some] = (p_buf[some, core].astype(F32) + r1_buf[some].astype(F32)).astype(BF)
        return carry

    lax.fori_loop(0, c_ssem.shape[0], join, 0)

    def scatter(order):
        out = []
        live = [(0, 0, 0)]
        for d in order:
            live = [plus(o, d, k) for o in live for k in range(dims[d])]
        for stage, d in enumerate(order):
            for offset in live:
                k = offset[d]
                if k:
                    i = index_of(plus(plus(offset, d, -k), d, -k))
                    cp = remote(
                        acc_buf.at[index_of(shifted(offset))],
                        r_buf.at[i],
                        s_ssem.at[i],
                        s_rsem.at[i],
                        device(along(d, k)),
                    )
                    cp.start()
                    out.append(cp)
            live = [o for o in live if o[d] == 0]
            last = stage == len(order) - 1
            for offset in live:
                b = index_of(shifted(offset))
                value = acc_buf[b].astype(F32)
                for k in range(1, dims[d]):
                    i = index_of(plus(offset, d, k))
                    remote(r_buf.at[i], r_buf.at[i], s_ssem.at[i], s_rsem.at[i], (s, other)).wait_recv()
                    value = value + r_buf[i].astype(F32)
                if last:
                    out_ref[...] = (mid_buf[...] + 0.5 * value).astype(BF)
                else:
                    acc_buf[b] = value.astype(BF)
        for cp in out:
            cp.wait_send()

    @pl.when(core == 0)
    def _():
        scatter((2, 1, 0))

    @pl.when(core == 1)
    def _():
        scatter((1, 0, 2))

    for cp in sends:
        cp.wait_send()


def fused_layer(
    zs,
    resid_in,
    query_plain,
    query_turn,
    latent_raw,
    shared_key,
    latent_gain,
    key_up,
    value_up,
    out_weight,
    mixer_gain,
    gate_weight,
    up_weight,
    down_weight,
):
    sp = lax.axis_size("sp")
    tp = lax.axis_size("tp")
    ys = sp // zs
    xs = tp // 2
    rows, width = resid_in.shape
    part = rows // tp
    hid = down_weight.shape[0] // sp
    cols = down_weight.shape[1]
    kv = latent_raw.shape[1]
    heads_width = query_plain.shape[1]
    position = (lax.axis_index("sp") * rows + jnp.arange(rows, dtype=jnp.int32)).astype(F32)
    inverse = 10000.0 ** (-jnp.arange(0, ROPE, 2, dtype=F32) / ROPE)
    inverse_lanes = jnp.tile(inverse, 128 * 2 // ROPE)
    angles = position[:, None] * inverse_lanes[None, :]
    sign = jnp.where(jnp.arange(128) % ROPE < ROPE // 2, -1.0, 1.0).astype(F32)
    cosine = jnp.cos(angles)
    sine = jnp.sin(angles) * sign[None, :]
    to_send = jnp.concatenate(
        [
            gate_weight.T.reshape(sp, hid, cols),
            up_weight.T.reshape(sp, hid, cols),
            down_weight.reshape(sp, hid, cols),
        ],
        axis=1,
    )
    groups = zs * ys * xs
    chunks = math.gcd(groups, 4)
    dma = pltpu.SemaphoreType.DMA
    vmem = lambda *shape: pltpu.VMEM(shape, BF)
    return pl.pallas_call(
        functools.partial(layer_kernel, (sp, tp, zs, ys, xs)),
        out_shape=jax.ShapeDtypeStruct((part, width), BF),
        in_specs=[pl.BlockSpec(memory_space=pltpu.VMEM)] * 13,
        out_specs=pl.BlockSpec(memory_space=pltpu.VMEM),
        scratch_shapes=[
            vmem(sp, 2, rows // 2, kv + 128),
            vmem(sp * rows, heads_width),
            vmem(sp * rows, heads_width),
            vmem(rows, heads_width),
            pltpu.VMEM((rows, width), F32),
            vmem(tp, part, width),
            vmem(tp, part, width),
            pltpu.VMEM((part, width), F32),
            vmem(3 * hid, width),
            vmem(groups, 2, part, width),
            vmem(groups, 2, part, width),
            vmem(groups, part, width),
            vmem(groups, part, width),
            vmem(groups, part, width),
            dma((sp,)),
            dma((sp,)),
            dma,
            dma((sp,)),
            dma((sp,)),
            dma((sp,)),
            dma((sp,)),
            dma((tp,)),
            dma((tp,)),
            dma((groups,)),
            dma((groups,)),
            dma((groups,)),
            dma((groups,)),
            dma((chunks,)),
            dma((chunks,)),
            dma((groups,)),
            dma((groups,)),
        ],
        compiler_params=pltpu.CompilerParams(has_side_effects=True, vmem_limit_bytes=60 * 1024 * 1024),
    )(
        resid_in,
        query_plain,
        query_turn,
        latent_raw,
        jnp.tile(shared_key, (1, 128 // ROPE)),
        cosine,
        sine,
        latent_gain[None, :],
        key_up,
        value_up,
        out_weight,
        mixer_gain[None, :],
        to_send,
    )


def per_device(*arrays):
    resid_in, query_plain, query_turn, latent_raw = arrays[:4]
    down_weight = arrays[-1]
    sp = lax.axis_size("sp")
    tp = lax.axis_size("tp")
    rows = resid_in.shape[0]
    fits = (
        sp % 2 == 0
        and tp % 2 == 0
        and rows % (32 * tp) == 0
        and down_weight.shape[0] % (16 * sp) == 0
        and down_weight.shape[1] % 128 == 0
        and latent_raw.shape[1] % 128 == 0
        and query_plain.shape[1] % 128 == 0
        and query_turn.shape[1] % 128 == 0
        and rows * sp <= 1024
        and sp * tp <= 32
    )
    if fits:
        return fused_layer(sp // 2, *arrays)
    return plain_layer(*arrays)


def solution(mesh):
    return jax.shard_map(
        per_device,
        mesh=mesh,
        in_specs=(
            P("sp", None),
            P("sp", "tp"),
            P("sp", "tp"),
            P("sp", None),
            P("sp", None),
            P(),
            P(None, "tp"),
            P(None, "tp"),
            P("tp", None),
            P(),
            P("sp", "tp"),
            P("sp", "tp"),
            P("tp", "sp"),
        ),
        out_specs=P(("sp", "tp"), None),
        check_vma=False,
    )
```

```python
import functools
import math

import jax
import jax.numpy as jnp
from jax import lax
from jax.experimental import pallas as pl
from jax.experimental.pallas import tpu as pltpu
from jax.sharding import PartitionSpec as P

NOPE = 64
ROPE = 32
V = 64


def rotate(values, cosine, sine):
    half_width = values.shape[-1] // 2
    first = values[..., :half_width]
    second = values[..., half_width:]
    return jnp.concatenate(
        [first * cosine - second * sine, first * sine + second * cosine], axis=-1
    )


def rms_scale(values, gain):
    return values * lax.rsqrt(jnp.mean(values * values, axis=-1, keepdims=True) + 1e-06) * gain


def plain_layer(
    resid_in,
    query_plain,
    query_turn,
    latent_raw,
    shared_key,
    latent_gain,
    key_up,
    value_up,
    out_weight,
    mixer_gain,
    gate_weight,
    up_weight,
    down_weight,
):
    tok_rows = resid_in.shape[0]
    head_count = query_plain.shape[1] // NOPE
    part_rows = tok_rows // lax.axis_size("tp")
    offset = lax.axis_index("sp") * tok_rows
    position = (offset + jnp.arange(tok_rows, dtype=jnp.int32)).astype(jnp.float32)
    inverse = 10000.0 ** (-jnp.arange(0, ROPE, 2, dtype=jnp.float32) / ROPE)
    angles = position[:, None] * inverse[None, :]
    cosine = jnp.cos(angles)
    sine = jnp.sin(angles)
    query_heads = query_plain.reshape(tok_rows, head_count, NOPE)
    query_rot = rotate(
        query_turn.reshape(tok_rows, head_count, ROPE).astype(jnp.float32),
        cosine[:, None, :],
        sine[:, None, :],
    ).astype(jnp.bfloat16)
    latent = rms_scale(latent_raw.astype(jnp.float32), latent_gain).astype(jnp.bfloat16)
    key_rot = rotate(shared_key.astype(jnp.float32), cosine, sine).astype(jnp.bfloat16)
    softmax_scale = (NOPE + ROPE) ** (-0.5)

    def attend_block(state, key_plain, values, key_pos):
        run_max, run_total, run_acc = state
        score = jnp.einsum(
            "qhd,khd->hqk", query_heads, key_plain, preferred_element_type=jnp.float32
        )
        score = score + jnp.einsum(
            "qhr,kr->hqk", query_rot, key_pos, preferred_element_type=jnp.float32
        )
        score = score * softmax_scale
        new_max = jnp.maximum(run_max, jnp.max(score, axis=-1))
        shrink = jnp.exp(run_max - new_max)
        expo = jnp.exp(score - new_max[:, :, None])
        run_total = run_total * shrink + jnp.sum(expo, axis=-1)
        run_acc = run_acc * shrink.T[:, :, None] + jnp.einsum(
            "hqk,khd->qhd", expo.astype(jnp.bfloat16), values, preferred_element_type=jnp.float32
        )
        return (new_max, run_total, run_acc)

    start_state = (
        jnp.full((head_count, tok_rows), -jnp.inf, jnp.float32),
        jnp.zeros((head_count, tok_rows), jnp.float32),
        jnp.zeros((tok_rows, head_count, V), jnp.float32),
    )
    state = start_state
    latent_piece = lax.all_gather(latent, "sp", axis=0, tiled=True)
    pos_piece = lax.all_gather(key_rot, "sp", axis=0, tiled=True)
    piece_len = latent_piece.shape[0]
    block_len = math.gcd(piece_len, 512)
    block_count = piece_len // block_len

    def one_block(inner, items):
        latent_rows, pos_rows = items
        key_plain = (
            jnp.dot(latent_rows, key_up, preferred_element_type=jnp.float32)
            .astype(jnp.bfloat16)
            .reshape(block_len, head_count, NOPE)
        )
        values = (
            jnp.dot(latent_rows, value_up, preferred_element_type=jnp.float32)
            .astype(jnp.bfloat16)
            .reshape(block_len, head_count, V)
        )
        return (attend_block(inner, key_plain, values, pos_rows), None)

    state, unused = lax.scan(
        one_block,
        state,
        (
            latent_piece.reshape(block_count, block_len, latent_piece.shape[1]),
            pos_piece.reshape(block_count, block_len, ROPE),
        ),
    )
    attended = (
        (state[2] / state[1].T[:, :, None]).astype(jnp.bfloat16).reshape(tok_rows, head_count * V)
    )
    own_start = lax.axis_index("tp") * part_rows
    mixed = lax.psum_scatter(
        jnp.dot(attended, out_weight, preferred_element_type=jnp.float32).astype(jnp.bfloat16),
        "tp",
        scatter_dimension=0,
        tiled=True,
    ).astype(jnp.float32)
    middle = lax.dynamic_slice_in_dim(resid_in, own_start, part_rows, 0).astype(jnp.float32) + mixed
    normed = rms_scale(middle, mixer_gain).astype(jnp.bfloat16)
    all_rows = lax.all_gather(normed, "tp", axis=0, tiled=True)
    gate_sum = jnp.dot(
        all_rows,
        lax.all_gather(gate_weight, "sp", axis=0, tiled=True),
        preferred_element_type=jnp.float32,
    )
    up_sum = jnp.dot(
        all_rows,
        lax.all_gather(up_weight, "sp", axis=0, tiled=True),
        preferred_element_type=jnp.float32,
    )
    hidden = (jax.nn.silu(gate_sum) * up_sum).astype(jnp.bfloat16)
    terms = jnp.dot(
        hidden,
        lax.all_gather(down_weight, "sp", axis=1, tiled=True),
        preferred_element_type=jnp.float32,
    )
    down_sum = lax.psum_scatter(
        terms.astype(jnp.bfloat16), "tp", scatter_dimension=0, tiled=True
    ).astype(jnp.float32)
    return (middle + 0.5 * down_sum).astype(jnp.bfloat16)

MESH = pl.DeviceIdType.MESH
BF = jnp.bfloat16
F32 = jnp.float32
BY_LAST = (((1,), (1,)), ((), ()))


def turn(values, cosine, sine):
    width = values.shape[-1]
    half = ROPE // 2
    lane = lax.broadcasted_iota(jnp.int32, values.shape, 1) % ROPE
    swapped = jnp.where(lane < half, pltpu.roll(values, width - half, 1), pltpu.roll(values, half, 1))
    return values * cosine + swapped * sine


def layer_kernel(
    sizes,
    resid_ref,
    query_ref,
    turn_ref,
    latent_ref,
    shared_ref,
    cos_ref,
    sin_ref,
    lgain_ref,
    kup_ref,
    vup_ref,
    ow_ref,
    mgain_ref,
    gate_ref,
    up_ref,
    down_ref,
    out_ref,
    kv_buf,
    key_buf,
    val_buf,
    att_buf,
    mix_buf,
    mixb_buf,
    mixr_buf,
    mid_buf,
    w_buf,
    n_buf,
    p_buf,
    r1_buf,
    acc_buf,
    r_buf,
    w_ssem,
    w_rsem,
    w_lsem,
    l_ssem,
    l_rsem,
    f_ssem,
    f_rsem,
    m_ssem,
    m_rsem,
    a_ssem,
    a_rsem,
    d_ssem,
    d_rsem,
    c_ssem,
    c_rsem,
    s_ssem,
    s_rsem,
):
    sp, tp, dims = sizes
    axes = range(len(dims))
    ring_dims, tp_dims = dims[:-1], dims[-1]
    s = lax.axis_index("sp")
    t = lax.axis_index("tp")
    core = t % 2
    other = t + 1 - 2 * core
    me = ()
    rest = s
    for size in reversed(ring_dims):
        me = (rest % size,) + me
        rest = rest // size
    me = me + (t // 2,)
    rows = latent_ref.shape[0]
    part = rows // tp
    hid, cols = gate_ref.shape[1:]
    kv_width = latent_ref.shape[1]

    def remote(src, dst, ssem, rsem, dev):
        return pltpu.make_async_remote_copy(
            src_ref=src, dst_ref=dst, send_sem=ssem, recv_sem=rsem, device_id=dev, device_id_type=MESH
        )

    sends = []

    lat = latent_ref[...].astype(F32)
    lat = lat * lax.rsqrt(jnp.mean(lat * lat, axis=-1, keepdims=True) + 1e-06) * lgain_ref[...]
    cosine = cos_ref[...]
    sine = sin_ref[...]
    half_rows = rows // 2
    own_lat = lat.astype(BF)
    own_key = turn(shared_ref[...].astype(F32), cosine, sine).astype(BF)
    for half in range(2):
        part_of = slice(half * half_rows, (half + 1) * half_rows)
        kv_buf[0, half, :, :kv_width] = own_lat[part_of]
        kv_buf[0, half, :, kv_width:] = own_key[part_of]
    for k in range(1, sp):
        cp = remote(kv_buf.at[0, core], kv_buf.at[k, core], l_ssem.at[k], l_rsem.at[k], ((s + k) % sp, t))
        cp.start()
        sends.append(cp)
    def index_of(place):
        index = 0
        for p, size in zip(place, dims):
            index = index * size + p
        return index

    def shifted(offset):
        return tuple((m + o) % n for m, o, n in zip(me, offset, dims))

    def device(offset):
        place = shifted(offset)
        ring = 0
        for p, size in zip(place, ring_dims):
            ring = ring * size + p
        return (ring, place[-1] * 2 + core)

    def along(d, k):
        return tuple(k if i == d else 0 for i in axes)

    def plus(offset, d, k):
        return tuple((o + k) % dims[d] if i == d else o for i, o in enumerate(offset))

    def offsets(sizes_of):
        found = [()]
        for size in sizes_of:
            found = [f + (k,) for f in found for k in range(size)]
        return found

    parts_of_w = (gate_ref, up_ref, down_ref)

    def w_slot(which):
        return w_buf.at[which * hid:(which + 1) * hid, pl.ds(pl.multiple_of(s * cols, cols), cols)]

    keeps = [
        pltpu.make_async_copy(ref.at[s], w_slot(which), w_lsem.at[which])
        for which, ref in enumerate(parts_of_w)
    ]
    for keep in keeps:
        keep.start()
    ring = sorted(offsets(ring_dims)[1:], reverse=True)
    late = [[o for o in ring if o[0]][-1], ring[-1]]
    early = [o for o in ring if o not in late]

    def send_weights(some, out):
        for offset in some:
            dest = device(offset + (0,))
            i = index_of(offset + (0,)) // tp_dims
            for which, ref in enumerate(parts_of_w):
                cp = remote(
                    ref.at[dest[0]], w_slot(which), w_ssem.at[which, i], w_rsem.at[which, i], dest
                )
                cp.start()
                out.append(cp)

    send_weights(early, sends)

    def make_kv(k):
        piece = kv_buf[k].reshape(rows, kv_buf.shape[3])
        piece_lat = piece[:, :kv_width]
        key_buf[k * rows:(k + 1) * rows, :] = jnp.dot(
            piece_lat, kup_ref[...], preferred_element_type=F32
        ).astype(BF)
        val_buf[k * rows:(k + 1) * rows, :] = jnp.dot(
            piece_lat, vup_ref[...], preferred_element_type=F32
        ).astype(BF)

    make_kv(0)
    query_rot = turn(
        turn_ref[...].astype(F32),
        jnp.concatenate([cosine] * (turn_ref.shape[1] // cosine.shape[1]), axis=1),
        jnp.concatenate([sine] * (turn_ref.shape[1] // cosine.shape[1]), axis=1),
    ).astype(BF)
    for k in range(1, sp):
        remote(kv_buf.at[k, core], kv_buf.at[k, core], l_ssem.at[k], l_rsem.at[k], (s, other)).wait_recv()
        cp = remote(kv_buf.at[k, core], kv_buf.at[k, core], f_ssem.at[k], f_rsem.at[k], (s, other))
        cp.start()
        sends.append(cp)
    for k in range(1, sp):
        remote(
            kv_buf.at[k, 1 - core], kv_buf.at[k, 1 - core], f_ssem.at[k], f_rsem.at[k], (s, other)
        ).wait_recv()
        make_kv(k)

    scale = (NOPE + ROPE) ** (-0.5)
    all_rot = kv_buf[...].reshape(sp * rows, kv_buf.shape[3])[:, kv_width:]
    lane = lax.broadcasted_iota(jnp.int32, (rows, 128), 1)
    for pair in range(query_ref.shape[1] // 128):
        span = slice(pair * 128, (pair + 1) * 128)
        keys = jnp.concatenate([key_buf[:, span], all_rot], axis=1)
        vals = val_buf[:, span]
        results = []
        for inner in range(2):
            head = pair * 2 + inner
            tile = head * ROPE // 128
            group = head % (128 // ROPE)
            q_plain = jnp.where(lane // NOPE == inner, query_ref[:, span], jnp.zeros((), BF))
            q_turn = jnp.where(
                lane // ROPE == group, query_rot[:, tile * 128:(tile + 1) * 128], jnp.zeros((), BF)
            )
            score = lax.dot_general(
                jnp.concatenate([q_plain, q_turn], axis=1), keys, BY_LAST, preferred_element_type=F32
            ) * scale
            top = jnp.max(score, axis=-1, keepdims=True)
            expo = jnp.exp(score - top)
            total = jnp.sum(expo, axis=-1, keepdims=True)
            results.append(jnp.dot(expo.astype(BF), vals, preferred_element_type=F32) / total)
        att_buf[:, span] = jnp.where(lane < V, results[0], results[1]).astype(BF)

    mix_buf[...] = jnp.dot(att_buf[...], ow_ref[...], preferred_element_type=F32)
    mixb_buf[...] = mix_buf[...].astype(BF).reshape(mixb_buf.shape)
    for j in range(1, tp):
        dest = (t + j) % tp
        cp = remote(mixb_buf.at[dest], mixr_buf.at[j], m_ssem.at[j], m_rsem.at[j], (s, dest))
        cp.start()
        sends.append(cp)
    own_rows = pl.ds(pl.multiple_of(t * part, part), part)
    mid = resid_ref[own_rows, :].astype(F32) + mix_buf[own_rows, :]
    for j in range(1, tp):
        remote(mixb_buf.at[0], mixr_buf.at[j], m_ssem.at[j], m_rsem.at[j], (s, other)).wait_recv()
        mid = mid + mixr_buf[j].astype(F32)
    mid_buf[...] = mid
    normed = mid * lax.rsqrt(jnp.mean(mid * mid, axis=-1, keepdims=True) + 1e-06) * mgain_ref[...]
    mine = index_of(me)
    n_buf[mine, core] = normed.astype(BF)

    def gather(order):
        held = [((0,) * len(dims), -1)]
        out = []
        for stage, d in enumerate(order):
            for offset, _ in list(held):
                for k in range(1, dims[d]):
                    held.append((plus(offset, d, k), stage))
        for offset, stage in held:
            block = n_buf.at[index_of(shifted(offset)), core]
            if stage >= 0:
                i = index_of(offset)
                remote(block, block, a_ssem.at[i], a_rsem.at[i], (s, other)).wait_recv()
            for d in order[stage + 1:]:
                for k in range(1, dims[d]):
                    i = index_of(plus(offset, d, -k))
                    cp = remote(block, block, a_ssem.at[i], a_rsem.at[i], device(along(d, k)))
                    cp.start()
                    out.append(cp)
            i = index_of(offset)
            cp = remote(block, block, d_ssem.at[i], d_rsem.at[i], (s, other))
            cp.start()
            out.append(cp)
            if stage < 0:
                send_weights(late, out)
        for offset, _ in held:
            i = index_of(offset)
            block = n_buf.at[index_of(shifted(offset)), 1 - core]
            remote(block, block, d_ssem.at[i], d_rsem.at[i], (s, other)).wait_recv()
        for cp in out:
            cp.wait_send()

    def feed_forward(order):
        for keep in keeps:
            keep.wait()
        for i in range(1, sp):
            for which in range(3):
                piece = w_buf.at[which * hid:(which + 1) * hid, :cols]
                remote(piece, piece, w_ssem.at[which, i], w_rsem.at[which, i], (s, other)).wait_recv()
        out = []
        zero = (0,) * len(dims)
        inner = offsets(dims[2:])
        step = len(inner)
        chunks = sorted(offsets(dims[:2]), key=lambda o: (o[1] == 0, o[0] == 0))

        def send(offset, d):
            i = index_of(plus(plus(offset, d, -offset[d]), d, -offset[d]))
            cp = remote(
                acc_buf.at[index_of(shifted(offset))], r_buf.at[i], s_ssem.at[i], s_rsem.at[i],
                device(along(d, offset[d])),
            )
            cp.start()
            out.append(cp)

        def across(g, outer):
            base = index_of(shifted(outer + zero[2:])[:2] + zero[2:])
            some = pl.ds(base, step)
            return some, remote(
                p_buf.at[some, 1 - core], r1_buf.at[some], c_ssem.at[g], c_rsem.at[g], (s, other)
            )

        def join(g, outer):
            some, cp = across(g, outer)
            cp.wait()
            acc_buf[some] = (p_buf[some, core].astype(F32) + r1_buf[some].astype(F32)).astype(BF)
            for o in inner:
                if (outer + o)[order[0]]:
                    send(outer + o, order[0])

        for g, outer in enumerate(chunks):
            some, cp = across(g, outer)
            block = n_buf[some].reshape(step * 2 * part, n_buf.shape[3])
            gate = lax.dot_general(block, w_buf[:hid], BY_LAST, preferred_element_type=F32)
            up = lax.dot_general(block, w_buf[hid:2 * hid], BY_LAST, preferred_element_type=F32)
            hidden = (gate / (1.0 + jnp.exp(-gate)) * up).astype(BF)
            down = jnp.dot(hidden, w_buf[2 * hid:], preferred_element_type=F32)
            p_buf[some] = down.astype(BF).reshape(step, 2, part, n_buf.shape[3])
            cp.start()
            if g:
                join(g - 1, chunks[g - 1])
        join(len(chunks) - 1, chunks[-1])

        live = [outer + o for outer in chunks for o in inner]
        for stage, d in enumerate(order):
            last = stage == len(order) - 1
            live = [o for o in live if o[d] == 0]
            if not last:
                live = [o for o in live if o[order[stage + 1]]] + [o for o in live if not o[order[stage + 1]]]
            for offset in live:
                b = index_of(shifted(offset))
                value = acc_buf[b].astype(F32)
                for k in range(1, dims[d]):
                    i = index_of(plus(offset, d, k))
                    remote(r_buf.at[i], r_buf.at[i], s_ssem.at[i], s_rsem.at[i], (s, other)).wait_recv()
                    value = value + r_buf[i].astype(F32)
                if last:
                    out_ref[...] = (mid_buf[...] + 0.5 * value).astype(BF)
                else:
                    acc_buf[b] = value.astype(BF)
                    if offset[order[stage + 1]]:
                        send(offset, order[stage + 1])
        for cp in out:
            cp.wait_send()

    @pl.when(core == 0)
    def _():
        gather((0, 1, 2, 3))
        feed_forward((3, 2, 1, 0))

    @pl.when(core == 1)
    def _():
        gather((0, 1, 3, 2))
        feed_forward((2, 3, 1, 0))

    for cp in sends:
        cp.wait_send()


def fused_layer(
    resid_in,
    query_plain,
    query_turn,
    latent_raw,
    shared_key,
    latent_gain,
    key_up,
    value_up,
    out_weight,
    mixer_gain,
    gate_weight,
    up_weight,
    down_weight,
):
    sp = lax.axis_size("sp")
    tp = lax.axis_size("tp")
    dims = (2, sp // 4, 2, tp // 2)
    rows, width = resid_in.shape
    part = rows // tp
    hid = down_weight.shape[0] // sp
    cols = down_weight.shape[1]
    kv = latent_raw.shape[1]
    heads_width = query_plain.shape[1]
    position = (lax.axis_index("sp") * rows + jnp.arange(rows, dtype=jnp.int32)).astype(F32)
    inverse = 10000.0 ** (-jnp.arange(0, ROPE, 2, dtype=F32) / ROPE)
    inverse_lanes = jnp.tile(inverse, 128 * 2 // ROPE)
    angles = position[:, None] * inverse_lanes[None, :]
    sign = jnp.where(jnp.arange(128) % ROPE < ROPE // 2, -1.0, 1.0).astype(F32)
    cosine = jnp.cos(angles)
    sine = jnp.sin(angles) * sign[None, :]
    groups = sp * tp // 2
    chunks = dims[0] * dims[1]
    dma = pltpu.SemaphoreType.DMA
    vmem = lambda *shape: pltpu.VMEM(shape, BF)
    return pl.pallas_call(
        functools.partial(layer_kernel, (sp, tp, dims)),
        out_shape=jax.ShapeDtypeStruct((part, width), BF),
        in_specs=[pl.BlockSpec(memory_space=pltpu.VMEM)] * 15,
        out_specs=pl.BlockSpec(memory_space=pltpu.VMEM),
        scratch_shapes=[
            vmem(sp, 2, rows // 2, kv + 128),
            vmem(sp * rows, heads_width),
            vmem(sp * rows, heads_width),
            vmem(rows, heads_width),
            pltpu.VMEM((rows, width), F32),
            vmem(tp, part, width),
            vmem(tp, part, width),
            pltpu.VMEM((part, width), F32),
            vmem(3 * hid, width),
            vmem(groups, 2, part, width),
            vmem(groups, 2, part, width),
            vmem(groups, part, width),
            vmem(groups, part, width),
            vmem(groups, part, width),
            dma((3, sp)),
            dma((3, sp)),
            dma((3,)),
            dma((sp,)),
            dma((sp,)),
            dma((sp,)),
            dma((sp,)),
            dma((tp,)),
            dma((tp,)),
            dma((groups,)),
            dma((groups,)),
            dma((groups,)),
            dma((groups,)),
            dma((chunks,)),
            dma((chunks,)),
            dma((groups,)),
            dma((groups,)),
        ],
        compiler_params=pltpu.CompilerParams(has_side_effects=True, vmem_limit_bytes=60 * 1024 * 1024),
    )(
        resid_in,
        query_plain,
        query_turn,
        latent_raw,
        jnp.tile(shared_key, (1, 128 // ROPE)),
        cosine,
        sine,
        latent_gain[None, :],
        key_up,
        value_up,
        out_weight,
        mixer_gain[None, :],
        gate_weight.T.reshape(sp, hid, cols),
        up_weight.T.reshape(sp, hid, cols),
        down_weight.reshape(sp, hid, cols),
    )


def per_device(*arrays):
    resid_in, query_plain, query_turn, latent_raw = arrays[:4]
    down_weight = arrays[-1]
    sp = lax.axis_size("sp")
    tp = lax.axis_size("tp")
    rows = resid_in.shape[0]
    fits = (
        sp % 4 == 0
        and tp % 2 == 0
        and rows % (32 * tp) == 0
        and down_weight.shape[0] % (16 * sp) == 0
        and down_weight.shape[1] % 128 == 0
        and latent_raw.shape[1] % 128 == 0
        and query_plain.shape[1] % 128 == 0
        and query_turn.shape[1] % 128 == 0
        and rows * sp <= 1024
        and sp * tp <= 32
    )
    if fits:
        return fused_layer(*arrays)
    return plain_layer(*arrays)


def solution(mesh):
    return jax.shard_map(
        per_device,
        mesh=mesh,
        in_specs=(
            P("sp", None),
            P("sp", "tp"),
            P("sp", "tp"),
            P("sp", None),
            P("sp", None),
            P(),
            P(None, "tp"),
            P(None, "tp"),
            P("tp", None),
            P(),
            P("sp", "tp"),
            P("sp", "tp"),
            P("tp", "sp"),
        ),
        out_specs=P(("sp", "tp"), None),
        check_vma=False,
    )
```

```python
import functools
import math

import jax
import jax.numpy as jnp
from jax import lax
from jax.experimental import pallas as pl
from jax.experimental.pallas import tpu as pltpu
from jax.sharding import PartitionSpec as P

NOPE = 64
ROPE = 32
V = 64


def rotate(values, cosine, sine):
    half_width = values.shape[-1] // 2
    first = values[..., :half_width]
    second = values[..., half_width:]
    return jnp.concatenate(
        [first * cosine - second * sine, first * sine + second * cosine], axis=-1
    )


def rms_scale(values, gain):
    return values * lax.rsqrt(jnp.mean(values * values, axis=-1, keepdims=True) + 1e-06) * gain


def plain_layer(
    resid_in,
    query_plain,
    query_turn,
    latent_raw,
    shared_key,
    latent_gain,
    key_up,
    value_up,
    out_weight,
    mixer_gain,
    gate_weight,
    up_weight,
    down_weight,
):
    tok_rows = resid_in.shape[0]
    head_count = query_plain.shape[1] // NOPE
    part_rows = tok_rows // lax.axis_size("tp")
    offset = lax.axis_index("sp") * tok_rows
    position = (offset + jnp.arange(tok_rows, dtype=jnp.int32)).astype(jnp.float32)
    inverse = 10000.0 ** (-jnp.arange(0, ROPE, 2, dtype=jnp.float32) / ROPE)
    angles = position[:, None] * inverse[None, :]
    cosine = jnp.cos(angles)
    sine = jnp.sin(angles)
    query_heads = query_plain.reshape(tok_rows, head_count, NOPE)
    query_rot = rotate(
        query_turn.reshape(tok_rows, head_count, ROPE).astype(jnp.float32),
        cosine[:, None, :],
        sine[:, None, :],
    ).astype(jnp.bfloat16)
    latent = rms_scale(latent_raw.astype(jnp.float32), latent_gain).astype(jnp.bfloat16)
    key_rot = rotate(shared_key.astype(jnp.float32), cosine, sine).astype(jnp.bfloat16)
    softmax_scale = (NOPE + ROPE) ** (-0.5)

    def attend_block(state, key_plain, values, key_pos):
        run_max, run_total, run_acc = state
        score = jnp.einsum(
            "qhd,khd->hqk", query_heads, key_plain, preferred_element_type=jnp.float32
        )
        score = score + jnp.einsum(
            "qhr,kr->hqk", query_rot, key_pos, preferred_element_type=jnp.float32
        )
        score = score * softmax_scale
        new_max = jnp.maximum(run_max, jnp.max(score, axis=-1))
        shrink = jnp.exp(run_max - new_max)
        expo = jnp.exp(score - new_max[:, :, None])
        run_total = run_total * shrink + jnp.sum(expo, axis=-1)
        run_acc = run_acc * shrink.T[:, :, None] + jnp.einsum(
            "hqk,khd->qhd", expo.astype(jnp.bfloat16), values, preferred_element_type=jnp.float32
        )
        return (new_max, run_total, run_acc)

    start_state = (
        jnp.full((head_count, tok_rows), -jnp.inf, jnp.float32),
        jnp.zeros((head_count, tok_rows), jnp.float32),
        jnp.zeros((tok_rows, head_count, V), jnp.float32),
    )
    state = start_state
    latent_piece = lax.all_gather(latent, "sp", axis=0, tiled=True)
    pos_piece = lax.all_gather(key_rot, "sp", axis=0, tiled=True)
    piece_len = latent_piece.shape[0]
    block_len = math.gcd(piece_len, 512)
    block_count = piece_len // block_len

    def one_block(inner, items):
        latent_rows, pos_rows = items
        key_plain = (
            jnp.dot(latent_rows, key_up, preferred_element_type=jnp.float32)
            .astype(jnp.bfloat16)
            .reshape(block_len, head_count, NOPE)
        )
        values = (
            jnp.dot(latent_rows, value_up, preferred_element_type=jnp.float32)
            .astype(jnp.bfloat16)
            .reshape(block_len, head_count, V)
        )
        return (attend_block(inner, key_plain, values, pos_rows), None)

    state, unused = lax.scan(
        one_block,
        state,
        (
            latent_piece.reshape(block_count, block_len, latent_piece.shape[1]),
            pos_piece.reshape(block_count, block_len, ROPE),
        ),
    )
    attended = (
        (state[2] / state[1].T[:, :, None]).astype(jnp.bfloat16).reshape(tok_rows, head_count * V)
    )
    own_start = lax.axis_index("tp") * part_rows
    mixed = lax.psum_scatter(
        jnp.dot(attended, out_weight, preferred_element_type=jnp.float32).astype(jnp.bfloat16),
        "tp",
        scatter_dimension=0,
        tiled=True,
    ).astype(jnp.float32)
    middle = lax.dynamic_slice_in_dim(resid_in, own_start, part_rows, 0).astype(jnp.float32) + mixed
    normed = rms_scale(middle, mixer_gain).astype(jnp.bfloat16)
    all_rows = lax.all_gather(normed, "tp", axis=0, tiled=True)
    gate_sum = jnp.dot(
        all_rows,
        lax.all_gather(gate_weight, "sp", axis=0, tiled=True),
        preferred_element_type=jnp.float32,
    )
    up_sum = jnp.dot(
        all_rows,
        lax.all_gather(up_weight, "sp", axis=0, tiled=True),
        preferred_element_type=jnp.float32,
    )
    hidden = (jax.nn.silu(gate_sum) * up_sum).astype(jnp.bfloat16)
    terms = jnp.dot(
        hidden,
        lax.all_gather(down_weight, "sp", axis=1, tiled=True),
        preferred_element_type=jnp.float32,
    )
    down_sum = lax.psum_scatter(
        terms.astype(jnp.bfloat16), "tp", scatter_dimension=0, tiled=True
    ).astype(jnp.float32)
    return (middle + 0.5 * down_sum).astype(jnp.bfloat16)

MESH = pl.DeviceIdType.MESH
BF = jnp.bfloat16
F32 = jnp.float32
BY_LAST = (((1,), (1,)), ((), ()))


def turn(values, cosine, sine):
    width = values.shape[-1]
    half = ROPE // 2
    lane = lax.broadcasted_iota(jnp.int32, values.shape, 1) % ROPE
    swapped = jnp.where(lane < half, pltpu.roll(values, width - half, 1), pltpu.roll(values, half, 1))
    return values * cosine + swapped * sine


def layer_kernel(
    sizes,
    resid_ref,
    query_ref,
    turn_ref,
    latent_ref,
    shared_ref,
    cos_ref,
    sin_ref,
    lgain_ref,
    kup_ref,
    vup_ref,
    ow_ref,
    mgain_ref,
    gate_ref,
    up_ref,
    down_ref,
    out_ref,
    kv_buf,
    key_buf,
    val_buf,
    att_buf,
    mix_buf,
    mixb_buf,
    mixr_buf,
    mid_buf,
    w_buf,
    n_buf,
    p_buf,
    r1_buf,
    acc_buf,
    r_buf,
    w_ssem,
    w_rsem,
    w_lsem,
    l_ssem,
    l_rsem,
    f_ssem,
    f_rsem,
    m_ssem,
    m_rsem,
    a_ssem,
    a_rsem,
    d_ssem,
    d_rsem,
    c_ssem,
    c_rsem,
    s_ssem,
    s_rsem,
):
    sp, tp, dims = sizes
    axes = range(len(dims))
    ring_dims, tp_dims = dims[:-1], dims[-1]
    s = lax.axis_index("sp")
    t = lax.axis_index("tp")
    core = t % 2
    other = t + 1 - 2 * core
    me = ()
    rest = s
    for size in reversed(ring_dims):
        me = (rest % size,) + me
        rest = rest // size
    me = me + (t // 2,)
    rows = latent_ref.shape[0]
    part = rows // tp
    hid, cols = gate_ref.shape[1:]
    kv_width = latent_ref.shape[1]

    def remote(src, dst, ssem, rsem, dev):
        return pltpu.make_async_remote_copy(
            src_ref=src, dst_ref=dst, send_sem=ssem, recv_sem=rsem, device_id=dev, device_id_type=MESH
        )

    sends = []

    lat = latent_ref[...].astype(F32)
    lat = lat * lax.rsqrt(jnp.mean(lat * lat, axis=-1, keepdims=True) + 1e-06) * lgain_ref[...]
    cosine = cos_ref[...]
    sine = sin_ref[...]
    half_rows = rows // 2
    own_lat = lat.astype(BF)
    own_key = turn(shared_ref[...].astype(F32), cosine, sine).astype(BF)
    for half in range(2):
        part_of = slice(half * half_rows, (half + 1) * half_rows)
        kv_buf[0, half, :, :kv_width] = own_lat[part_of]
        kv_buf[0, half, :, kv_width:] = own_key[part_of]
    for k in range(1, sp):
        cp = remote(kv_buf.at[0, core], kv_buf.at[k, core], l_ssem.at[k], l_rsem.at[k], ((s + k) % sp, t))
        cp.start()
        sends.append(cp)
    def index_of(place):
        index = 0
        for p, size in zip(place, dims):
            index = index * size + p
        return index

    def shifted(offset):
        return tuple((m + o) % n for m, o, n in zip(me, offset, dims))

    def device(offset):
        place = shifted(offset)
        ring = 0
        for p, size in zip(place, ring_dims):
            ring = ring * size + p
        return (ring, place[-1] * 2 + core)

    def along(d, k):
        return tuple(k if i == d else 0 for i in axes)

    def plus(offset, d, k):
        return tuple((o + k) % dims[d] if i == d else o for i, o in enumerate(offset))

    def offsets(sizes_of):
        found = [()]
        for size in sizes_of:
            found = [f + (k,) for f in found for k in range(size)]
        return found

    parts_of_w = (gate_ref, up_ref, down_ref)

    def w_slot(which):
        return w_buf.at[which * hid:(which + 1) * hid, pl.ds(pl.multiple_of(s * cols, cols), cols)]

    keeps = [
        pltpu.make_async_copy(ref.at[s], w_slot(which), w_lsem.at[which])
        for which, ref in enumerate(parts_of_w)
    ]
    for keep in keeps:
        keep.start()
    ring = sorted(offsets(ring_dims)[1:], reverse=True)
    late = [o for o in ring if o[0]][-2:] + ring[-3:]
    early = [o for o in ring if o not in late]

    def send_weights(some, out):
        for which, ref in enumerate(parts_of_w):
            for offset in some:
                dest = device(offset + (0,))
                i = index_of(offset + (0,)) // tp_dims
                cp = remote(
                    ref.at[dest[0]], w_slot(which), w_ssem.at[which, i], w_rsem.at[which, i], dest
                )
                cp.start()
                out.append(cp)

    send_weights(early, sends)

    def make_kv(k):
        piece = kv_buf[k].reshape(rows, kv_buf.shape[3])
        piece_lat = piece[:, :kv_width]
        key_buf[k * rows:(k + 1) * rows, :] = jnp.dot(
            piece_lat, kup_ref[...], preferred_element_type=F32
        ).astype(BF)
        val_buf[k * rows:(k + 1) * rows, :] = jnp.dot(
            piece_lat, vup_ref[...], preferred_element_type=F32
        ).astype(BF)

    make_kv(0)
    query_rot = turn(
        turn_ref[...].astype(F32),
        jnp.concatenate([cosine] * (turn_ref.shape[1] // cosine.shape[1]), axis=1),
        jnp.concatenate([sine] * (turn_ref.shape[1] // cosine.shape[1]), axis=1),
    ).astype(BF)
    for k in range(1, sp):
        remote(kv_buf.at[k, core], kv_buf.at[k, core], l_ssem.at[k], l_rsem.at[k], (s, other)).wait_recv()
        cp = remote(kv_buf.at[k, core], kv_buf.at[k, core], f_ssem.at[k], f_rsem.at[k], (s, other))
        cp.start()
        sends.append(cp)
    for k in range(1, sp):
        remote(
            kv_buf.at[k, 1 - core], kv_buf.at[k, 1 - core], f_ssem.at[k], f_rsem.at[k], (s, other)
        ).wait_recv()
        make_kv(k)

    scale = (NOPE + ROPE) ** (-0.5)
    all_rot = kv_buf[...].reshape(sp * rows, kv_buf.shape[3])[:, kv_width:]
    lane = lax.broadcasted_iota(jnp.int32, (rows, 128), 1)
    for pair in range(query_ref.shape[1] // 128):
        span = slice(pair * 128, (pair + 1) * 128)
        keys = jnp.concatenate([key_buf[:, span], all_rot], axis=1)
        vals = val_buf[:, span]
        results = []
        for inner in range(2):
            head = pair * 2 + inner
            tile = head * ROPE // 128
            group = head % (128 // ROPE)
            q_plain = jnp.where(lane // NOPE == inner, query_ref[:, span], jnp.zeros((), BF))
            q_turn = jnp.where(
                lane // ROPE == group, query_rot[:, tile * 128:(tile + 1) * 128], jnp.zeros((), BF)
            )
            score = lax.dot_general(
                jnp.concatenate([q_plain, q_turn], axis=1), keys, BY_LAST, preferred_element_type=F32
            ) * scale
            top = jnp.max(score, axis=-1, keepdims=True)
            expo = jnp.exp(score - top)
            total = jnp.sum(expo, axis=-1, keepdims=True)
            results.append(jnp.dot(expo.astype(BF), vals, preferred_element_type=F32) / total)
        att_buf[:, span] = jnp.where(lane < V, results[0], results[1]).astype(BF)

    mix_buf[...] = jnp.dot(att_buf[...], ow_ref[...], preferred_element_type=F32)
    mixb_buf[...] = mix_buf[...].astype(BF).reshape(mixb_buf.shape)
    for j in range(1, tp):
        dest = (t + j) % tp
        cp = remote(mixb_buf.at[dest], mixr_buf.at[j], m_ssem.at[j], m_rsem.at[j], (s, dest))
        cp.start()
        sends.append(cp)
    own_rows = pl.ds(pl.multiple_of(t * part, part), part)
    mid = resid_ref[own_rows, :].astype(F32) + mix_buf[own_rows, :]
    for j in range(1, tp):
        remote(mixb_buf.at[0], mixr_buf.at[j], m_ssem.at[j], m_rsem.at[j], (s, other)).wait_recv()
        mid = mid + mixr_buf[j].astype(F32)
    mid_buf[...] = mid
    normed = mid * lax.rsqrt(jnp.mean(mid * mid, axis=-1, keepdims=True) + 1e-06) * mgain_ref[...]
    mine = index_of(me)
    n_buf[mine, core] = normed.astype(BF)

    def gather(order):
        held = [((0,) * len(dims), -1)]
        out = []
        for stage, d in enumerate(order):
            for offset, _ in list(held):
                for k in range(1, dims[d]):
                    held.append((plus(offset, d, k), stage))
        for offset, stage in held:
            block = n_buf.at[index_of(shifted(offset)), core]
            if stage >= 0:
                i = index_of(offset)
                remote(block, block, a_ssem.at[i], a_rsem.at[i], (s, other)).wait_recv()
            for d in order[stage + 1:]:
                for k in range(1, dims[d]):
                    i = index_of(plus(offset, d, -k))
                    cp = remote(block, block, a_ssem.at[i], a_rsem.at[i], device(along(d, k)))
                    cp.start()
                    out.append(cp)
            i = index_of(offset)
            cp = remote(block, block, d_ssem.at[i], d_rsem.at[i], (s, other))
            cp.start()
            out.append(cp)
            if stage == 0:
                send_weights(late, out)
        for offset, _ in held:
            i = index_of(offset)
            block = n_buf.at[index_of(shifted(offset)), 1 - core]
            remote(block, block, d_ssem.at[i], d_rsem.at[i], (s, other)).wait_recv()
        for cp in out:
            cp.wait_send()

    def feed_forward(order):
        def arrived(which):
            keeps[which].wait()
            piece = w_buf.at[which * hid:(which + 1) * hid, :cols]
            for i in range(1, sp):
                remote(piece, piece, w_ssem.at[which, i], w_rsem.at[which, i], (s, other)).wait_recv()

        arrived(0)
        arrived(1)
        out = []
        zero = (0,) * len(dims)
        inner = offsets(dims[2:])
        step = len(inner)
        chunks = sorted(offsets(dims[:2]), key=lambda o: (o[1] == 0, o[0] == 0))

        def send(offset, d):
            i = index_of(plus(plus(offset, d, -offset[d]), d, -offset[d]))
            cp = remote(
                acc_buf.at[index_of(shifted(offset))], r_buf.at[i], s_ssem.at[i], s_rsem.at[i],
                device(along(d, offset[d])),
            )
            cp.start()
            out.append(cp)

        def across(g, outer):
            base = index_of(shifted(outer + zero[2:])[:2] + zero[2:])
            some = pl.ds(base, step)
            return some, remote(
                p_buf.at[some, 1 - core], r1_buf.at[some], c_ssem.at[g], c_rsem.at[g], (s, other)
            )

        def join(g, outer):
            some, cp = across(g, outer)
            cp.wait()
            acc_buf[some] = (p_buf[some, core].astype(F32) + r1_buf[some].astype(F32)).astype(BF)
            for o in inner:
                if (outer + o)[order[0]]:
                    send(outer + o, order[0])

        for g, outer in enumerate(chunks):
            some, cp = across(g, outer)
            block = n_buf[some].reshape(step * 2 * part, n_buf.shape[3])
            gate = lax.dot_general(block, w_buf[:hid], BY_LAST, preferred_element_type=F32)
            up = lax.dot_general(block, w_buf[hid:2 * hid], BY_LAST, preferred_element_type=F32)
            hidden = (gate / (1.0 + jnp.exp(-gate)) * up).astype(BF)
            if g == 0:
                arrived(2)
            down = jnp.dot(hidden, w_buf[2 * hid:], preferred_element_type=F32)
            p_buf[some] = down.astype(BF).reshape(step, 2, part, n_buf.shape[3])
            cp.start()
            if g:
                join(g - 1, chunks[g - 1])
        join(len(chunks) - 1, chunks[-1])

        live = [outer + o for outer in chunks for o in inner]
        for stage, d in enumerate(order):
            last = stage == len(order) - 1
            live = [o for o in live if o[d] == 0]
            if not last:
                live = [o for o in live if o[order[stage + 1]]] + [o for o in live if not o[order[stage + 1]]]
            for offset in live:
                b = index_of(shifted(offset))
                value = acc_buf[b].astype(F32)
                for k in range(1, dims[d]):
                    i = index_of(plus(offset, d, k))
                    remote(r_buf.at[i], r_buf.at[i], s_ssem.at[i], s_rsem.at[i], (s, other)).wait_recv()
                    value = value + r_buf[i].astype(F32)
                if last:
                    out_ref[...] = (mid_buf[...] + 0.5 * value).astype(BF)
                else:
                    acc_buf[b] = value.astype(BF)
                    if offset[order[stage + 1]]:
                        send(offset, order[stage + 1])
        for cp in out:
            cp.wait_send()

    @pl.when(core == 0)
    def _():
        gather((0, 1, 2, 3))
        feed_forward((3, 2, 1, 0))

    @pl.when(core == 1)
    def _():
        gather((0, 1, 2, 3))
        feed_forward((2, 3, 1, 0))

    for cp in sends:
        cp.wait_send()


def fused_layer(
    resid_in,
    query_plain,
    query_turn,
    latent_raw,
    shared_key,
    latent_gain,
    key_up,
    value_up,
    out_weight,
    mixer_gain,
    gate_weight,
    up_weight,
    down_weight,
):
    sp = lax.axis_size("sp")
    tp = lax.axis_size("tp")
    dims = (2, sp // 4, 2, tp // 2)
    rows, width = resid_in.shape
    part = rows // tp
    hid = down_weight.shape[0] // sp
    cols = down_weight.shape[1]
    kv = latent_raw.shape[1]
    heads_width = query_plain.shape[1]
    position = (lax.axis_index("sp") * rows + jnp.arange(rows, dtype=jnp.int32)).astype(F32)
    inverse = 10000.0 ** (-jnp.arange(0, ROPE, 2, dtype=F32) / ROPE)
    inverse_lanes = jnp.tile(inverse, 128 * 2 // ROPE)
    angles = position[:, None] * inverse_lanes[None, :]
    sign = jnp.where(jnp.arange(128) % ROPE < ROPE // 2, -1.0, 1.0).astype(F32)
    cosine = jnp.cos(angles)
    sine = jnp.sin(angles) * sign[None, :]
    groups = sp * tp // 2
    chunks = dims[0] * dims[1]
    dma = pltpu.SemaphoreType.DMA
    vmem = lambda *shape: pltpu.VMEM(shape, BF)
    return pl.pallas_call(
        functools.partial(layer_kernel, (sp, tp, dims)),
        out_shape=jax.ShapeDtypeStruct((part, width), BF),
        in_specs=[pl.BlockSpec(memory_space=pltpu.VMEM)] * 15,
        out_specs=pl.BlockSpec(memory_space=pltpu.VMEM),
        scratch_shapes=[
            vmem(sp, 2, rows // 2, kv + 128),
            vmem(sp * rows, heads_width),
            vmem(sp * rows, heads_width),
            vmem(rows, heads_width),
            pltpu.VMEM((rows, width), F32),
            vmem(tp, part, width),
            vmem(tp, part, width),
            pltpu.VMEM((part, width), F32),
            vmem(3 * hid, width),
            vmem(groups, 2, part, width),
            vmem(groups, 2, part, width),
            vmem(groups, part, width),
            vmem(groups, part, width),
            vmem(groups, part, width),
            dma((3, sp)),
            dma((3, sp)),
            dma((3,)),
            dma((sp,)),
            dma((sp,)),
            dma((sp,)),
            dma((sp,)),
            dma((tp,)),
            dma((tp,)),
            dma((groups,)),
            dma((groups,)),
            dma((groups,)),
            dma((groups,)),
            dma((chunks,)),
            dma((chunks,)),
            dma((groups,)),
            dma((groups,)),
        ],
        compiler_params=pltpu.CompilerParams(has_side_effects=True, vmem_limit_bytes=60 * 1024 * 1024),
    )(
        resid_in,
        query_plain,
        query_turn,
        latent_raw,
        jnp.tile(shared_key, (1, 128 // ROPE)),
        cosine,
        sine,
        latent_gain[None, :],
        key_up,
        value_up,
        out_weight,
        mixer_gain[None, :],
        gate_weight.T.reshape(sp, hid, cols),
        up_weight.T.reshape(sp, hid, cols),
        down_weight.reshape(sp, hid, cols),
    )


def per_device(*arrays):
    resid_in, query_plain, query_turn, latent_raw = arrays[:4]
    down_weight = arrays[-1]
    sp = lax.axis_size("sp")
    tp = lax.axis_size("tp")
    rows = resid_in.shape[0]
    fits = (
        sp % 4 == 0
        and tp % 2 == 0
        and rows % (32 * tp) == 0
        and down_weight.shape[0] % (16 * sp) == 0
        and down_weight.shape[1] % 128 == 0
        and latent_raw.shape[1] % 128 == 0
        and query_plain.shape[1] % 128 == 0
        and query_turn.shape[1] % 128 == 0
        and rows * sp <= 1024
        and sp * tp <= 32
    )
    if fits:
        return fused_layer(*arrays)
    return plain_layer(*arrays)


def solution(mesh):
    return jax.shard_map(
        per_device,
        mesh=mesh,
        in_specs=(
            P("sp", None),
            P("sp", "tp"),
            P("sp", "tp"),
            P("sp", None),
            P("sp", None),
            P(),
            P(None, "tp"),
            P(None, "tp"),
            P("tp", None),
            P(),
            P("sp", "tp"),
            P("sp", "tp"),
            P("tp", "sp"),
        ),
        out_specs=P(("sp", "tp"), None),
        check_vma=False,
    )
```
